32 devices in a mesh: grp: 2 (over y), kv: 4 (over z), tp: 4 (over x, core).
Axes of the slice: x: 2, y: 2, z: 4, core: 2. Of those that a mesh axis runs over, the one named last changes fastest.
Arguments:
- tokens: bfloat16 [32, 2048], P('grp', ('kv', 'tp')), parts along dimension 0, may hold values from -13 to 13, as said below
- state: float32 [32, 16, 128, 128], P(('grp', 'kv'), 'tp'), parts along dimension 0, may hold values from -0.6 to 0.6
- norm_gain: bfloat16 [2048], P('kv'), may hold values from 0.099609375 to 1.8984375
- w_query: bfloat16 [2048, 2048], P('kv', 'tp'), may hold values from -0.125 to 0.125
- w_key: bfloat16 [2048, 2048], P('kv', 'tp'), may hold values from -0.125 to 0.125
- w_value: bfloat16 [2048, 2048], P('kv', 'tp'), may hold values from -0.125 to 0.125
- w_beta: bfloat16 [2048, 16], replicated, may hold values from -0.125 to 0.125
- w_decay: bfloat16 [2048, 16], replicated, may hold values from -0.125 to 0.125
- a_log: float32 [16], P('tp'), may hold values from -3 to 1
- dt_bias: float32 [16], P('tp'), may hold values from -2 to 1
- head_gain: float32 [128], replicated, may hold values from 0.1 to 1.9
- w_out: bfloat16 [2048, 2048], P('tp', 'kv'), may hold values from -0.125 to 0.125
- mixer_gain: bfloat16 [2048], P('kv'), may hold values from 0.099609375 to 1.8984375
- w_up: bfloat16 [2048, 8192], P('kv', 'tp'), may hold values from -0.125 to 0.125
- w_down: bfloat16 [8192, 2048], P('tp', 'kv'), may hold values from -0.0625 to 0.0625
Outputs:
- mixed: bfloat16 [32, 2048], P('grp', ('kv', 'tp')), parts along dimension 0
- new_state: float32 [32, 16, 128, 128], P(('grp', 'kv'), 'tp'), parts along dimension 0
The draws below stay inside these ranges and needn't reach their ends.
There are 2 independent parts, one for each index of `grp`. The reference program is written for one: setup_inputs(seed, part) draws one part's arguments, and reference() takes and returns one part's arrays. A program takes and returns all parts, laid end to end along the dimension named above; an argument that names none is the same for every part. Nothing has to cross between parts.
Inputs may be any that keep to these rules, and one draw needn't show every extreme that they name: `tokens`: activations of order one.
All inputs are finite; a program needn't handle non-finite values.
Results may differ from the reference program's by a relative error of at most 0.019.
Values may be sent and summed in bfloat16 or wider, within the bound.
A program may use at most 64 MiB of HBM per device.

```python
import jax
import jax.numpy as jnp
from jax import lax

D = 2048
HEADS = 16
HEAD = 128
FF = 8192
BATCH = 16
N_TP = 4


def draw_tokens(key, part):
    first_key, second_key = jax.random.split(jax.random.fold_in(key, 17), 2)
    ramp = jnp.exp(jnp.linspace(jnp.log(0.5), jnp.log(1.5), D)).astype(jnp.float32)
    rough = jnp.exp(jax.random.uniform(second_key, (1, D), jnp.float32, -0.35, 0.35))
    base = jnp.clip(jax.random.normal(first_key, (BATCH, D), jnp.float32), -6.0, 6.0)
    return (base * ramp * rough).astype(jnp.bfloat16)


def steps_of(rng, extent, shards, low, top_value):
    def one(dim, blocks):
        heights = jax.random.uniform(jax.random.fold_in(jax.random.fold_in(rng, 6), dim), (blocks,), jnp.float32, low / len(shards), top_value / len(shards))
        return jnp.repeat(jnp.exp(heights), extent[dim] // blocks).reshape((-1,) + (1,) * (len(extent) - dim - 1))

    loudness = one(*shards[0])
    for cut in shards[1:]:
        loudness = loudness * one(*cut)
    return loudness


def scatter_about(key, shape, spread, limit, cuts=(), held_as=jnp.bfloat16):
    array = spread * jax.random.normal(key, shape, jnp.float32)
    if cuts:
        array = array * steps_of(key, shape, cuts, -0.22, 0.18)
    return jnp.clip(array, -limit, limit).astype(held_as)


def setup_inputs(seed: int = 0, part: int = 0) -> dict:
    splits = jax.random.split(jax.random.key(seed), 16)
    own_keys = jax.random.split(jax.random.fold_in(splits[15], part), 16)
    tokens = draw_tokens(jax.random.fold_in(jax.random.fold_in(splits[15], part), 71), part)
    state = scatter_about(own_keys[1], (BATCH, HEADS, HEAD, HEAD), 0.1, 0.6, ((0, 4), (1, 4)), jnp.float32)
    norm_gain = jnp.clip(1.0 + 0.18 * jax.random.normal(splits[2], (D,), jnp.float32), 0.099609375, 1.8984375).astype(jnp.bfloat16)
    w_query = scatter_about(splits[3], (D, HEADS * HEAD), D ** -0.5, 0.125, ((0, 4), (1, 4)))
    w_key = scatter_about(splits[4], (D, HEADS * HEAD), D ** -0.5, 0.125, ((0, 4), (1, 4)))
    w_value = scatter_about(splits[5], (D, HEADS * HEAD), D ** -0.5, 0.125, ((0, 4), (1, 4)))
    w_beta = scatter_about(splits[6], (D, HEADS), D ** -0.5, 0.125)
    w_decay = scatter_about(splits[7], (D, HEADS), D ** -0.5, 0.125)
    a_log = jnp.clip(-3.0 + 4.0 * jax.random.uniform(splits[8], (HEADS,), jnp.float32) ** steps_of(splits[8], (HEADS,), ((0, 4),), -0.2, 0.2), -3.0, 1.0)
    dt_bias = jnp.clip(-2.0 + 3.0 * jax.random.uniform(splits[9], (HEADS,), jnp.float32) ** steps_of(splits[9], (HEADS,), ((0, 4),), -0.2, 0.2), -2.0, 1.0)
    head_gain = jnp.clip(1.0 + 0.18 * jax.random.normal(splits[10], (HEAD,), jnp.float32), 0.1, 1.9)
    w_out = scatter_about(splits[11], (HEADS * HEAD, D), (HEADS * HEAD) ** -0.5, 0.125, ((0, 4), (1, 4)))
    mixer_gain = jnp.clip(1.0 + 0.18 * jax.random.normal(splits[12], (D,), jnp.float32), 0.099609375, 1.8984375).astype(jnp.bfloat16)
    w_up = scatter_about(splits[13], (D, FF), D ** -0.5, 0.125, ((0, 4), (1, 4)))
    w_down = scatter_about(splits[14], (FF, D), FF ** -0.5, 0.0625, ((0, 4), (1, 4)))
    return {"tokens": tokens, "state": state, "norm_gain": norm_gain, "w_query": w_query, "w_key": w_key, "w_value": w_value, "w_beta": w_beta, "w_decay": w_decay, "a_log": a_log, "dt_bias": dt_bias, "head_gain": head_gain, "w_out": w_out, "mixer_gain": mixer_gain, "w_up": w_up, "w_down": w_down}


epsilon = 1e-06

def dotted(left, right):
    return jnp.dot(left, right, preferred_element_type=jnp.float32)

def delta_update(query_pre, key_pre, value_pre, beta_pre, decay_pre, state, a_log, dt_bias, head_gain):
    query = query_pre * lax.rsqrt(lax.optimization_barrier(jnp.sum(query_pre * query_pre, axis=-1, keepdims=True)) + epsilon)
    keyed = key_pre * lax.rsqrt(lax.optimization_barrier(jnp.sum(key_pre * key_pre, axis=-1, keepdims=True)) + epsilon)
    beta = jax.nn.sigmoid(beta_pre)
    decay = jnp.exp(-jnp.exp(a_log) * jax.nn.softplus(decay_pre + dt_bias))
    key_read = jnp.einsum('bhk,bhkv->bhv', keyed, state)
    query_read = jnp.einsum('bhk,bhkv->bhv', query, state)
    fresh = beta[..., None] * (value_pre - decay[..., None] * key_read)
    new_state = decay[..., None, None] * state + keyed[..., :, None] * fresh[..., None, :]
    intersection = lax.optimization_barrier(jnp.sum(query * keyed, axis=-1))
    reading = decay[..., None] * query_read + intersection[..., None] * fresh
    normed = reading * lax.rsqrt(lax.optimization_barrier(jnp.mean(reading * reading, axis=-1, keepdims=True)) + epsilon) * head_gain
    return (normed.astype(jnp.bfloat16), new_state)

def grouped_sum(left, weight, groups):
    rows = left.shape[0]
    width = left.shape[1] // groups
    left_g = left.reshape(rows, groups, width).astype(jnp.float32)
    weight_g = weight.reshape(groups, width, weight.shape[1]).astype(jnp.float32)
    partial_g = jnp.einsum('bgi,gio->bgo', left_g, weight_g)
    return lax.optimization_barrier(jnp.sum(partial_g.astype(jnp.bfloat16).astype(jnp.float32), axis=1))

def reference(tokens, state, norm_gain, w_query, w_key, w_value, w_beta, w_decay, a_log, dt_bias, head_gain, w_out, mixer_gain, w_up, w_down):
    rows = tokens.shape[0]
    inputs = tokens.astype(jnp.float32)
    first = lax.rsqrt(lax.optimization_barrier(jnp.mean(inputs * inputs, axis=-1, keepdims=True)) + epsilon)
    scaled = (inputs * norm_gain.astype(jnp.float32)).astype(jnp.bfloat16)
    query_pre = (first * dotted(scaled, w_query)).reshape(rows, HEADS, HEAD)
    key_pre = (first * dotted(scaled, w_key)).reshape(rows, HEADS, HEAD)
    value_pre = (first * dotted(scaled, w_value)).reshape(rows, HEADS, HEAD)
    beta_pre = first * dotted(scaled, w_beta)
    decay_pre = first * dotted(scaled, w_decay)
    normed, new_state = delta_update(query_pre, key_pre, value_pre, beta_pre, decay_pre, state, a_log, dt_bias, head_gain)
    attended = grouped_sum(normed.reshape(rows, HEADS * HEAD), w_out, N_TP)
    middle = (inputs + attended).astype(jnp.bfloat16)
    middle_f = middle.astype(jnp.float32)
    second = lax.rsqrt(lax.optimization_barrier(jnp.mean(middle_f * middle_f, axis=-1, keepdims=True)) + epsilon)
    scaled_two = (middle_f * mixer_gain.astype(jnp.float32)).astype(jnp.bfloat16)
    hidden = jnp.square(jax.nn.relu(second * dotted(scaled_two, w_up))).astype(jnp.bfloat16)
    lowered = grouped_sum(hidden, w_down, N_TP)
    mixed = (middle_f + lowered).astype(jnp.bfloat16)
    return (mixed, new_state)
```

```python
import functools

import jax
import jax.numpy as jnp
from jax import lax
from jax.experimental import pallas as pl
from jax.experimental.pallas import tpu as pltpu
from jax.sharding import PartitionSpec as P

MESH = pl.DeviceIdType.MESH

epsilon = 1e-06


def dotted(left, right):
    return jnp.dot(left, right, preferred_element_type=jnp.float32)


def delta_update(
    query_pre, key_pre, value_pre, beta_pre, decay_pre, state, a_log, dt_bias, head_gain
):
    query = query_pre * lax.rsqrt(jnp.sum(query_pre * query_pre, axis=-1, keepdims=True) + epsilon)
    keyed = key_pre * lax.rsqrt(jnp.sum(key_pre * key_pre, axis=-1, keepdims=True) + epsilon)
    beta = jax.nn.sigmoid(beta_pre)
    decay = jnp.exp(-jnp.exp(a_log) * jax.nn.softplus(decay_pre + dt_bias))
    key_read = jnp.einsum("bhk,bhkv->bhv", keyed, state)
    query_read = jnp.einsum("bhk,bhkv->bhv", query, state)
    fresh = beta[..., None] * (value_pre - decay[..., None] * key_read)
    new_state = decay[..., None, None] * state + keyed[..., :, None] * fresh[..., None, :]
    intersection = jnp.sum(query * keyed, axis=-1)
    reading = decay[..., None] * query_read + intersection[..., None] * fresh
    normed = (
        reading
        * lax.rsqrt(jnp.mean(reading * reading, axis=-1, keepdims=True) + epsilon)
        * head_gain
    )
    return (normed.astype(jnp.bfloat16), new_state)


def by_collectives(
    tokens,
    state,
    norm_gain,
    w_query,
    w_key,
    w_value,
    w_beta,
    w_decay,
    a_log,
    dt_bias,
    head_gain,
    w_out,
    mixer_gain,
    w_up,
    w_down,
):
    seq_here = state.shape[0]
    heads_here = state.shape[1]
    head_size = state.shape[2]
    kv_index = lax.axis_index("kv")
    tp_index = lax.axis_index("tp")
    gathered = lax.all_gather(tokens, "tp", axis=1, tiled=True)
    block = gathered.shape[1]
    width = block * lax.axis_size("kv")
    inputs = gathered.astype(jnp.float32)
    scaled = (inputs * norm_gain.astype(jnp.float32)).astype(jnp.bfloat16)
    partial_sq = jnp.sum(inputs * inputs, axis=1)
    beta_rows = lax.dynamic_slice(
        w_beta, (kv_index * block, tp_index * heads_here), (block, heads_here)
    )
    decay_rows = lax.dynamic_slice(
        w_decay, (kv_index * block, tp_index * heads_here), (block, heads_here)
    )
    query_part = dotted(scaled, w_query)
    key_part = dotted(scaled, w_key)
    value_part = dotted(scaled, w_value)
    beta_part = dotted(scaled, beta_rows)
    decay_part = dotted(scaled, decay_rows)
    square_all = lax.psum(partial_sq, "kv")
    square_sum = lax.dynamic_slice_in_dim(square_all, kv_index * seq_here, seq_here, 0)
    query_sum, key_sum, value_sum, beta_sum, decay_sum = (
        lax.psum_scatter(query_part, "kv", scatter_dimension=0, tiled=True),
        lax.psum_scatter(key_part, "kv", scatter_dimension=0, tiled=True),
        lax.psum_scatter(value_part, "kv", scatter_dimension=0, tiled=True),
        lax.psum_scatter(beta_part, "kv", scatter_dimension=0, tiled=True),
        lax.psum_scatter(decay_part, "kv", scatter_dimension=0, tiled=True),
    )
    first = lax.rsqrt(square_sum / width + epsilon)[:, None]
    query_pre = (first * query_sum).reshape(seq_here, heads_here, head_size)
    key_pre = (first * key_sum).reshape(seq_here, heads_here, head_size)
    value_pre = (first * value_sum).reshape(seq_here, heads_here, head_size)
    normed, new_state = delta_update(
        query_pre,
        key_pre,
        value_pre,
        first * beta_sum,
        first * decay_sum,
        state,
        a_log,
        dt_bias,
        head_gain,
    )
    normed = normed.reshape(seq_here, heads_here * head_size)
    head_part = dotted(lax.all_gather(normed, "kv", axis=0, tiled=True), w_out)
    attended = lax.psum_scatter(
        head_part.astype(jnp.bfloat16), "tp", scatter_dimension=1, tiled=True
    ).astype(jnp.float32)
    middle = (tokens.astype(jnp.float32) + attended).astype(jnp.bfloat16)
    middle_rows = lax.all_gather(middle, "tp", axis=1, tiled=True).astype(jnp.float32)
    square_two = lax.psum(jnp.sum(middle_rows * middle_rows, axis=1), "kv")
    second = lax.rsqrt(square_two / width + epsilon)[:, None]
    scaled_two = (middle_rows * mixer_gain.astype(jnp.float32)).astype(jnp.bfloat16)
    up_part = dotted(scaled_two, w_up)
    up_share = lax.psum_scatter(up_part, "kv", scatter_dimension=1, tiled=True)
    hidden_share = jnp.square(jax.nn.relu(second * up_share)).astype(jnp.bfloat16)
    down_part = dotted(lax.all_gather(hidden_share, "kv", axis=1, tiled=True), w_down)
    lowered = lax.psum_scatter(
        down_part.astype(jnp.bfloat16), "tp", scatter_dimension=1, tiled=True
    ).astype(jnp.float32)
    mixed = (middle.astype(jnp.float32) + lowered).astype(jnp.bfloat16)
    return (mixed, new_state)


def across(left, right):
    return lax.dot_general(
        left, right, (((1,), (1,)), ((), ())), preferred_element_type=jnp.float32
    )


def layer_kernel(
    n_kv,
    n_tp,
    tokens,
    state,
    norm_gain,
    w_query,
    w_key,
    w_value,
    w_beta,
    w_decay,
    a_log,
    dt_bias,
    head_gain,
    w_out,
    mixer_gain,
    w_up,
    w_down,
    mixed,
    new_state,
    token_all,
    gain_one,
    gain_two,
    gain_head,
    query_w,
    key_w,
    value_w,
    beta_w,
    decay_w,
    out_w,
    up_w,
    down_w,
    states,
    states_low,
    log_s,
    bias_s,
    qkv_send,
    qkv_recv,
    norm_all,
    part_all,
    middle_all,
    up_send,
    up_recv,
    hidden_all,
    down_send,
    down_recv,
    mixed_v,
    load_sem,
    store_sem,
    tp_send_sem,
    tp_recv_sem,
    kv_send_sem,
    kv_recv_sem,
):
    f32, bf16 = jnp.float32, jnp.bfloat16
    kv = lax.axis_index("kv")
    tp = lax.axis_index("tp")
    rows, feats = tokens.shape
    block = n_tp * feats
    seqs, heads, size = state.shape[:3]
    pairs = seqs * heads
    all_heads = w_beta.shape[0]
    share = w_up.shape[1] // n_kv
    width = block * n_kv

    barrier = pltpu.get_barrier_semaphore()
    for off in range(1, n_tp):
        pl.semaphore_signal(
            barrier, inc=1, device_id={"tp": lax.rem(tp + off, n_tp)}, device_id_type=MESH
        )
    for off in range(1, n_kv):
        pl.semaphore_signal(
            barrier, inc=1, device_id={"kv": lax.rem(kv + off, n_kv)}, device_id_type=MESH
        )

    my_rows = pl.ds(pl.multiple_of(kv * block, block), block)
    loads = {}
    for number, (name, source, target) in enumerate(
        (
            ("tokens", tokens, token_all.at[tp]),
            ("gain_one", norm_gain, gain_one),
            ("query", w_query, query_w),
            ("key", w_key, key_w),
            ("value", w_value, value_w),
            ("beta", w_beta.at[:, my_rows], beta_w),
            ("decay", w_decay.at[:, my_rows], decay_w),
            ("log", a_log, log_s),
            ("bias", dt_bias, bias_s),
            ("gain_head", head_gain, gain_head),
            ("state", state, states),
            ("out", w_out, out_w),
            ("gain_two", mixer_gain, gain_two),
            ("up", w_up, up_w),
            ("down", w_down, down_w),
        )
    ):
        loads[name] = pltpu.make_async_copy(source, target, load_sem.at[number])
        loads[name].start()

    sends = []

    def over_tp(stage, off, source, target):
        copy = pltpu.make_async_remote_copy(
            src_ref=source,
            dst_ref=target,
            send_sem=tp_send_sem.at[stage, off - 1],
            recv_sem=tp_recv_sem.at[stage, off - 1],
            device_id={"tp": lax.rem(tp + off, n_tp)},
            device_id_type=MESH,
        )
        return copy

    def over_kv(stage, off, source, target):
        copy = pltpu.make_async_remote_copy(
            src_ref=source,
            dst_ref=target,
            send_sem=kv_send_sem.at[stage, off - 1],
            recv_sem=kv_recv_sem.at[stage, off - 1],
            device_id={"kv": lax.rem(kv + off, n_kv)},
            device_id_type=MESH,
        )
        return copy

    def gather(over, stage, here, count, slots):
        for off in range(1, count):
            copy = over(stage, off, slots.at[here], slots.at[here])
            copy.start()
            sends.append(copy)

    def arrived(over, stage, off, here, count, slots):
        origin = lax.rem(here + count - off, count)
        over(stage, off, slots.at[origin], slots.at[origin]).wait_recv()
        return origin

    loads["tokens"].wait()
    pl.semaphore_wait(barrier, n_tp + n_kv - 2)

    gather(over_tp, 0, tp, n_tp, token_all)
    for name in ("gain_one", "query", "key", "value", "beta", "decay", "log", "bias", "gain_head"):
        loads[name].wait()
    for off in range(1, n_tp):
        arrived(over_tp, 0, off, tp, n_tp, token_all)
    inputs = jnp.concatenate([token_all[t].astype(f32) for t in range(n_tp)], axis=1)
    scaled = (inputs * gain_one[...].astype(f32)).astype(bf16)
    square = jnp.sum(inputs * inputs, axis=1, keepdims=True)
    side = jnp.concatenate(
        [
            across(scaled, beta_w[...]),
            across(scaled, decay_w[...]),
            square,
            jnp.zeros((rows, 64 - 2 * all_heads - 1), f32),
        ],
        axis=1,
    )
    side_high = side.astype(bf16).astype(f32)
    side = jnp.concatenate([side_high, side - side_high], axis=1)
    parts = [dotted(scaled, w[...]) for w in (query_w, key_w, value_w)]
    pad = jnp.zeros((16 - seqs, 128), f32)
    for dest in range(n_kv):
        at = slice(dest * seqs, (dest + 1) * seqs)
        pieces = [p[at, h * size : (h + 1) * size] for p in parts for h in range(heads)]
        qkv_send[dest] = jnp.concatenate(pieces + [side[at], pad], axis=0).astype(bf16)
    for off in range(1, n_kv):
        copy = over_kv(0, off, qkv_send.at[lax.rem(kv + off, n_kv)], qkv_recv.at[off - 1])
        copy.start()
        sends.append(copy)

    loads["state"].wait()
    for b in range(seqs):
        for h in range(heads):
            states_low[h * seqs + b] = states[b, h].astype(bf16)
    total = qkv_send[kv].astype(f32)
    for off in range(1, n_kv):
        over_kv(0, off, qkv_recv.at[off - 1], qkv_recv.at[off - 1]).wait_recv()
        total = total + qkv_recv[off - 1].astype(f32)

    lane = lax.rem(lax.broadcasted_iota(jnp.int32, (pairs, 128), 1), 64)
    head = lax.broadcasted_iota(jnp.int32, (pairs, 128), 0) // seqs
    side = jnp.concatenate([total[3 * pairs : 3 * pairs + seqs]] * heads, axis=0)

    def column(index):
        return jnp.sum(jnp.where(lane == index, side, 0.0), axis=1, keepdims=True)

    head_one = lax.broadcasted_iota(jnp.int32, (pairs, 1), 0) // seqs
    log_rate = jnp.zeros((pairs, 1), f32)
    bias = jnp.zeros((pairs, 1), f32)
    for h in range(heads):
        log_rate = jnp.where(head_one == h, log_s[h], log_rate)
        bias = jnp.where(head_one == h, bias_s[h], bias)
    first = lax.rsqrt(column(2 * all_heads) / width + epsilon)
    logit = first * column(tp * heads + head)
    beta = 1.0 / (1.0 + jnp.exp(-logit))
    gate = first * column(all_heads + tp * heads + head) + bias
    softplus = jnp.maximum(gate, 0.0) + jnp.log1p(jnp.exp(-jnp.abs(gate)))
    decay = jnp.exp(-jnp.exp(log_rate) * softplus)
    query_pre = first * total[:pairs]
    key_pre = first * total[pairs : 2 * pairs]
    value_pre = first * total[2 * pairs : 3 * pairs]
    query = query_pre * lax.rsqrt(jnp.sum(query_pre * query_pre, axis=1, keepdims=True) + epsilon)
    keyed = key_pre * lax.rsqrt(jnp.sum(key_pre * key_pre, axis=1, keepdims=True) + epsilon)
    both = jnp.concatenate([keyed, query], axis=0).astype(bf16)
    pair = lax.rem(lax.broadcasted_iota(jnp.int32, (2 * pairs, size), 0), pairs)
    reads = jnp.zeros((2 * pairs, size), f32)
    for r in range(pairs):
        reads = jnp.where(pair == r, dotted(both, states_low[r]), reads)
    fresh = beta * (value_pre - decay * reads[:pairs])
    overlap = jnp.sum(query * keyed, axis=1, keepdims=True)
    reading = decay * reads[pairs:] + overlap * fresh
    scale = lax.rsqrt(jnp.sum(reading * reading, axis=1, keepdims=True) / size + epsilon)
    norm_all[kv] = (reading * scale * gain_head[...]).astype(bf16)
    gather(over_kv, 1, kv, n_kv, norm_all)

    key_columns = keyed.T
    for r in range(pairs):
        b, h = r % seqs, r // seqs
        outer = key_columns[:, r : r + 1] * fresh[r : r + 1, :]
        states[b, h] = decay[r : r + 1, :] * states[b, h] + outer
    store_state = pltpu.make_async_copy(states, new_state, store_sem.at[0])
    store_state.start()
    for name in ("out", "gain_two", "up", "down"):
        loads[name].wait()

    for off in range(1, n_kv):
        arrived(over_kv, 1, off, kv, n_kv, norm_all)
    normed = [norm_all[k].astype(f32) for k in range(n_kv)]
    normed = jnp.concatenate(
        [
            jnp.concatenate([x[h * seqs : (h + 1) * seqs] for x in normed], axis=0)
            for h in range(heads)
        ],
        axis=1,
    ).astype(bf16)
    part_all[tp] = dotted(normed, out_w[...]).astype(bf16)
    gather(over_tp, 1, tp, n_tp, part_all)
    for off in range(1, n_tp):
        arrived(over_tp, 1, off, tp, n_tp, part_all)
    attended = part_all[0].astype(f32)
    for t in range(1, n_tp):
        attended = attended + part_all[t].astype(f32)
    inputs = jnp.concatenate([token_all[t].astype(f32) for t in range(n_tp)], axis=1)
    middle = (inputs + attended).astype(bf16).astype(f32)
    for t in range(n_tp):
        middle_all[t] = middle[:, t * feats : (t + 1) * feats]
    square = jnp.sum(middle * middle, axis=1, keepdims=True)
    square_high = square.astype(bf16).astype(f32)
    lane = lax.broadcasted_iota(jnp.int32, (rows, 128), 1)
    square_pair = jnp.where(
        lane == 0, square_high, jnp.where(lane == 1, square - square_high, 0.0)
    ).astype(bf16)
    scaled = (middle * gain_two[...].astype(f32)).astype(bf16)

    def up_block(dest):
        at = pl.ds(pl.multiple_of(dest * share, share), share)
        return dotted(scaled, up_w[:, at])

    for off in range(1, n_kv):
        dest = lax.rem(kv + off, n_kv)
        up_send[off - 1, :, :share] = up_block(dest).astype(bf16)
        up_send[off - 1, :, share:] = square_pair
        copy = over_kv(2, off, up_send.at[off - 1], up_recv.at[off - 1])
        copy.start()
        sends.append(copy)
    up = up_block(kv)
    pair_sum = square_pair.astype(f32)
    for off in range(1, n_kv):
        over_kv(2, off, up_recv.at[off - 1], up_recv.at[off - 1]).wait_recv()
        up = up + up_recv[off - 1, :, :share].astype(f32)
        pair_sum = pair_sum + up_recv[off - 1, :, share:].astype(f32)
    second = lax.rsqrt(jnp.sum(pair_sum, axis=1, keepdims=True) / width + epsilon)
    hidden_all[kv] = jnp.square(jnp.maximum(second * up, 0.0)).astype(bf16)
    gather(over_kv, 3, kv, n_kv, hidden_all)

    def down_block(source):
        at = pl.ds(pl.multiple_of(source * share, share), share)
        return dotted(hidden_all[source], down_w[at, :])

    down = down_block(kv)
    for off in range(1, n_kv):
        down = down + down_block(arrived(over_kv, 3, off, kv, n_kv, hidden_all))
    for t in range(n_tp):
        down_send[t] = down[:, t * feats : (t + 1) * feats].astype(bf16)
    for off in range(1, n_tp):
        copy = over_tp(2, off, down_send.at[lax.rem(tp + off, n_tp)], down_recv.at[off - 1])
        copy.start()
        sends.append(copy)
    lowered = down_send[tp].astype(f32)
    for off in range(1, n_tp):
        over_tp(2, off, down_recv.at[off - 1], down_recv.at[off - 1]).wait_recv()
        lowered = lowered + down_recv[off - 1].astype(f32)
    mixed_v[...] = (middle_all[tp] + lowered).astype(bf16)
    store_mixed = pltpu.make_async_copy(mixed_v, mixed, store_sem.at[1])
    store_mixed.start()
    for copy in sends:
        copy.wait_send()
    store_state.wait()
    store_mixed.wait()


def local(n_kv, n_tp, *arrays):
    tokens, state, w_beta, w_up = arrays[0], arrays[1], arrays[6], arrays[13]
    rows, feats = tokens.shape
    seqs, heads, size = state.shape[:3]
    pairs = seqs * heads
    share = w_up.shape[1] // n_kv
    aligned = (
        rows % 16 == 0
        and feats % 128 == 0
        and size == 128
        and pairs % 16 == 0
        and seqs <= 16
        and seqs * n_kv == rows
        and 2 * w_beta.shape[1] < 64
        and share % 128 == 0
        and n_kv > 1
        and n_tp > 1
    )
    if not aligned:
        return by_collectives(*arrays)
    block = n_tp * feats
    bf16, f32 = jnp.bfloat16, jnp.float32
    vmem = pltpu.VMEM

    def held(array):
        return vmem(array.shape, array.dtype)

    norm_gain, w_query, w_key, w_value = arrays[2:6]
    head_gain, w_out, mixer_gain, w_up, w_down = arrays[10:]
    dma = pltpu.SemaphoreType.DMA
    return pl.pallas_call(
        functools.partial(layer_kernel, n_kv, n_tp),
        out_shape=(
            jax.ShapeDtypeStruct(tokens.shape, tokens.dtype),
            jax.ShapeDtypeStruct(state.shape, state.dtype),
        ),
        in_specs=[pl.BlockSpec(memory_space=pl.ANY)] * len(arrays),
        out_specs=(pl.BlockSpec(memory_space=pl.ANY),) * 2,
        scratch_shapes=[
            vmem((n_tp, rows, feats), bf16),
            held(norm_gain),
            held(mixer_gain),
            held(head_gain),
            held(w_query),
            held(w_key),
            held(w_value),
            vmem((w_beta.shape[1], block), bf16),
            vmem((w_beta.shape[1], block), bf16),
            held(w_out),
            held(w_up),
            held(w_down),
            held(state),
            vmem((pairs, size, size), bf16),
            pltpu.SMEM((heads,), f32),
            pltpu.SMEM((heads,), f32),
            vmem((n_kv, 3 * pairs + 16, size), bf16),
            vmem((n_kv - 1, 3 * pairs + 16, size), bf16),
            vmem((n_kv, pairs, size), bf16),
            vmem((n_tp, rows, block), bf16),
            vmem((n_tp, rows, feats), f32),
            vmem((n_kv - 1, rows, share + 128), bf16),
            vmem((n_kv - 1, rows, share + 128), bf16),
            vmem((n_kv, rows, share), bf16),
            vmem((n_tp, rows, feats), bf16),
            vmem((n_tp - 1, rows, feats), bf16),
            vmem((rows, feats), bf16),
            dma((15,)),
            dma((2,)),
            dma((3, n_tp - 1)),
            dma((3, n_tp - 1)),
            dma((4, n_kv - 1)),
            dma((4, n_kv - 1)),
        ],
        compiler_params=pltpu.CompilerParams(collective_id=0, has_side_effects=True),
    )(*arrays[:6], arrays[6].T, arrays[7].T, *arrays[8:])


def solution(mesh):
    return jax.shard_map(
        functools.partial(local, mesh.shape["kv"], mesh.shape["tp"]),
        mesh=mesh,
        in_specs=(
            P("grp", ("kv", "tp")),
            P(("grp", "kv"), "tp", None, None),
            P("kv"),
            P("kv", "tp"),
            P("kv", "tp"),
            P("kv", "tp"),
            P(),
            P(),
            P("tp"),
            P("tp"),
            P(),
            P("tp", "kv"),
            P("kv"),
            P("kv", "tp"),
            P("tp", "kv"),
        ),
        out_specs=(P("grp", ("kv", "tp")), P(("grp", "kv"), "tp", None, None)),
        check_vma=False,
    )
```

```python
import functools

import jax
import jax.numpy as jnp
from jax import lax
from jax.experimental import pallas as pl
from jax.experimental.pallas import tpu as pltpu
from jax.sharding import PartitionSpec as P

MESH = pl.DeviceIdType.MESH

epsilon = 1e-06


def dotted(left, right):
    return jnp.dot(left, right, preferred_element_type=jnp.float32)


def delta_update(
    query_pre, key_pre, value_pre, beta_pre, decay_pre, state, a_log, dt_bias, head_gain
):
    query = query_pre * lax.rsqrt(jnp.sum(query_pre * query_pre, axis=-1, keepdims=True) + epsilon)
    keyed = key_pre * lax.rsqrt(jnp.sum(key_pre * key_pre, axis=-1, keepdims=True) + epsilon)
    beta = jax.nn.sigmoid(beta_pre)
    decay = jnp.exp(-jnp.exp(a_log) * jax.nn.softplus(decay_pre + dt_bias))
    key_read = jnp.einsum("bhk,bhkv->bhv", keyed, state)
    query_read = jnp.einsum("bhk,bhkv->bhv", query, state)
    fresh = beta[..., None] * (value_pre - decay[..., None] * key_read)
    new_state = decay[..., None, None] * state + keyed[..., :, None] * fresh[..., None, :]
    intersection = jnp.sum(query * keyed, axis=-1)
    reading = decay[..., None] * query_read + intersection[..., None] * fresh
    normed = (
        reading
        * lax.rsqrt(jnp.mean(reading * reading, axis=-1, keepdims=True) + epsilon)
        * head_gain
    )
    return (normed.astype(jnp.bfloat16), new_state)


def by_collectives(
    tokens,
    state,
    norm_gain,
    w_query,
    w_key,
    w_value,
    w_beta,
    w_decay,
    a_log,
    dt_bias,
    head_gain,
    w_out,
    mixer_gain,
    w_up,
    w_down,
):
    seq_here = state.shape[0]
    heads_here = state.shape[1]
    head_size = state.shape[2]
    kv_index = lax.axis_index("kv")
    tp_index = lax.axis_index("tp")
    gathered = lax.all_gather(tokens, "tp", axis=1, tiled=True)
    block = gathered.shape[1]
    width = block * lax.axis_size("kv")
    inputs = gathered.astype(jnp.float32)
    scaled = (inputs * norm_gain.astype(jnp.float32)).astype(jnp.bfloat16)
    partial_sq = jnp.sum(inputs * inputs, axis=1)
    beta_rows = lax.dynamic_slice(
        w_beta, (kv_index * block, tp_index * heads_here), (block, heads_here)
    )
    decay_rows = lax.dynamic_slice(
        w_decay, (kv_index * block, tp_index * heads_here), (block, heads_here)
    )
    query_part = dotted(scaled, w_query)
    key_part = dotted(scaled, w_key)
    value_part = dotted(scaled, w_value)
    beta_part = dotted(scaled, beta_rows)
    decay_part = dotted(scaled, decay_rows)
    square_all = lax.psum(partial_sq, "kv")
    square_sum = lax.dynamic_slice_in_dim(square_all, kv_index * seq_here, seq_here, 0)
    query_sum, key_sum, value_sum, beta_sum, decay_sum = (
        lax.psum_scatter(query_part, "kv", scatter_dimension=0, tiled=True),
        lax.psum_scatter(key_part, "kv", scatter_dimension=0, tiled=True),
        lax.psum_scatter(value_part, "kv", scatter_dimension=0, tiled=True),
        lax.psum_scatter(beta_part, "kv", scatter_dimension=0, tiled=True),
        lax.psum_scatter(decay_part, "kv", scatter_dimension=0, tiled=True),
    )
    first = lax.rsqrt(square_sum / width + epsilon)[:, None]
    query_pre = (first * query_sum).reshape(seq_here, heads_here, head_size)
    key_pre = (first * key_sum).reshape(seq_here, heads_here, head_size)
    value_pre = (first * value_sum).reshape(seq_here, heads_here, head_size)
    normed, new_state = delta_update(
        query_pre,
        key_pre,
        value_pre,
        first * beta_sum,
        first * decay_sum,
        state,
        a_log,
        dt_bias,
        head_gain,
    )
    normed = normed.reshape(seq_here, heads_here * head_size)
    head_part = dotted(lax.all_gather(normed, "kv", axis=0, tiled=True), w_out)
    attended = lax.psum_scatter(
        head_part.astype(jnp.bfloat16), "tp", scatter_dimension=1, tiled=True
    ).astype(jnp.float32)
    middle = (tokens.astype(jnp.float32) + attended).astype(jnp.bfloat16)
    middle_rows = lax.all_gather(middle, "tp", axis=1, tiled=True).astype(jnp.float32)
    square_two = lax.psum(jnp.sum(middle_rows * middle_rows, axis=1), "kv")
    second = lax.rsqrt(square_two / width + epsilon)[:, None]
    scaled_two = (middle_rows * mixer_gain.astype(jnp.float32)).astype(jnp.bfloat16)
    up_part = dotted(scaled_two, w_up)
    up_share = lax.psum_scatter(up_part, "kv", scatter_dimension=1, tiled=True)
    hidden_share = jnp.square(jax.nn.relu(second * up_share)).astype(jnp.bfloat16)
    down_part = dotted(lax.all_gather(hidden_share, "kv", axis=1, tiled=True), w_down)
    lowered = lax.psum_scatter(
        down_part.astype(jnp.bfloat16), "tp", scatter_dimension=1, tiled=True
    ).astype(jnp.float32)
    mixed = (middle.astype(jnp.float32) + lowered).astype(jnp.bfloat16)
    return (mixed, new_state)


def across(left, right):
    return lax.dot_general(
        left, right, (((1,), (1,)), ((), ())), preferred_element_type=jnp.float32
    )


def layer_kernel(
    n_kv,
    n_tp,
    tokens,
    state,
    norm_gain,
    w_query,
    w_key,
    w_value,
    w_beta,
    w_decay,
    a_log,
    dt_bias,
    head_gain,
    w_out,
    mixer_gain,
    w_up,
    w_down,
    mixed,
    new_state,
    token_all,
    gain_one,
    gain_two,
    gain_head,
    query_w,
    key_w,
    value_w,
    beta_w,
    decay_w,
    out_w,
    up_w,
    down_w,
    states,
    states_low,
    log_s,
    bias_s,
    qkv_send,
    qkv_recv,
    norm_all,
    part_all,
    middle_all,
    up_send,
    up_recv,
    hidden_all,
    down_send,
    down_recv,
    load_sem,
    tp_send_sem,
    tp_recv_sem,
    kv_send_sem,
    kv_recv_sem,
):
    f32, bf16 = jnp.float32, jnp.bfloat16
    kv = lax.axis_index("kv")
    tp = lax.axis_index("tp")
    rows, feats = tokens.shape
    block = n_tp * feats
    seqs, heads, size = state.shape[:3]
    pairs = seqs * heads
    all_heads = w_beta.shape[0]
    share = w_up.shape[1] // n_kv
    width = block * n_kv

    barrier = pltpu.get_barrier_semaphore()
    for off in range(1, n_tp):
        pl.semaphore_signal(
            barrier, inc=1, device_id={"tp": lax.rem(tp + off, n_tp)}, device_id_type=MESH
        )
    for off in range(1, n_kv):
        pl.semaphore_signal(
            barrier, inc=1, device_id={"kv": lax.rem(kv + off, n_kv)}, device_id_type=MESH
        )

    my_rows = pl.ds(pl.multiple_of(kv * block, block), block)
    loads = {}
    for number, (name, source, target) in enumerate(
        (
            ("tokens", tokens, token_all.at[tp]),
            ("gain_one", norm_gain, gain_one),
            ("query", w_query, query_w),
            ("key", w_key, key_w),
            ("value", w_value, value_w),
            ("beta", w_beta.at[:, my_rows], beta_w),
            ("decay", w_decay.at[:, my_rows], decay_w),
            ("log", a_log, log_s),
            ("bias", dt_bias, bias_s),
            ("gain_head", head_gain, gain_head),
            ("state", state, states),
            ("out", w_out, out_w),
            ("gain_two", mixer_gain, gain_two),
            ("up", w_up, up_w),
            ("down", w_down, down_w),
        )
    ):
        loads[name] = pltpu.make_async_copy(source, target, load_sem.at[number])
        loads[name].start()

    sends = []

    def over_tp(stage, off, source, target):
        copy = pltpu.make_async_remote_copy(
            src_ref=source,
            dst_ref=target,
            send_sem=tp_send_sem.at[stage, off - 1],
            recv_sem=tp_recv_sem.at[stage, off - 1],
            device_id={"tp": lax.rem(tp + off, n_tp)},
            device_id_type=MESH,
        )
        return copy

    def over_kv(stage, off, source, target):
        copy = pltpu.make_async_remote_copy(
            src_ref=source,
            dst_ref=target,
            send_sem=kv_send_sem.at[stage, off - 1],
            recv_sem=kv_recv_sem.at[stage, off - 1],
            device_id={"kv": lax.rem(kv + off, n_kv)},
            device_id_type=MESH,
        )
        return copy

    def gather(over, stage, here, count, slots):
        for off in range(1, count):
            copy = over(stage, off, slots.at[here], slots.at[here])
            copy.start()
            sends.append(copy)

    def arrived(over, stage, off, here, count, slots):
        origin = lax.rem(here + count - off, count)
        over(stage, off, slots.at[origin], slots.at[origin]).wait_recv()
        return origin

    loads["tokens"].wait()
    pl.semaphore_wait(barrier, n_tp + n_kv - 2)

    gather(over_tp, 0, tp, n_tp, token_all)
    for name in ("gain_one", "query", "key", "value", "beta", "decay", "log", "bias", "gain_head"):
        loads[name].wait()
    for off in range(1, n_tp):
        arrived(over_tp, 0, off, tp, n_tp, token_all)
    inputs = jnp.concatenate([token_all[t].astype(f32) for t in range(n_tp)], axis=1)
    scaled = (inputs * gain_one[...].astype(f32)).astype(bf16)
    square = jnp.sum(inputs * inputs, axis=1, keepdims=True)
    side = jnp.concatenate(
        [
            across(scaled, beta_w[...]),
            across(scaled, decay_w[...]),
            square,
            jnp.zeros((rows, 64 - 2 * all_heads - 1), f32),
        ],
        axis=1,
    )
    side_high = side.astype(bf16).astype(f32)
    side = jnp.concatenate([side_high, side - side_high], axis=1)
    parts = [dotted(scaled, w[...]) for w in (query_w, key_w, value_w)]
    pad = jnp.zeros((16 - seqs, 128), f32)
    for dest in range(n_kv):
        at = slice(dest * seqs, (dest + 1) * seqs)
        pieces = [p[at, h * size : (h + 1) * size] for p in parts for h in range(heads)]
        qkv_send[dest] = jnp.concatenate(pieces + [side[at], pad], axis=0).astype(bf16)
    for off in range(1, n_kv):
        copy = over_kv(0, off, qkv_send.at[lax.rem(kv + off, n_kv)], qkv_recv.at[off - 1])
        copy.start()
        sends.append(copy)

    loads["state"].wait()
    for b in range(seqs):
        for h in range(heads):
            states_low[h * seqs + b] = states[b, h].astype(bf16)
    total = qkv_send[kv].astype(f32)
    for off in range(1, n_kv):
        over_kv(0, off, qkv_recv.at[off - 1], qkv_recv.at[off - 1]).wait_recv()
        total = total + qkv_recv[off - 1].astype(f32)

    lane = lax.rem(lax.broadcasted_iota(jnp.int32, (pairs, 128), 1), 64)
    head = lax.broadcasted_iota(jnp.int32, (pairs, 128), 0) // seqs
    side = jnp.concatenate([total[3 * pairs : 3 * pairs + seqs]] * heads, axis=0)

    def column(index):
        return jnp.sum(jnp.where(lane == index, side, 0.0), axis=1, keepdims=True)

    head_one = lax.broadcasted_iota(jnp.int32, (pairs, 1), 0) // seqs
    log_rate = jnp.zeros((pairs, 1), f32)
    bias = jnp.zeros((pairs, 1), f32)
    for h in range(heads):
        log_rate = jnp.where(head_one == h, log_s[h], log_rate)
        bias = jnp.where(head_one == h, bias_s[h], bias)
    first = lax.rsqrt(column(2 * all_heads) / width + epsilon)
    logit = first * column(tp * heads + head)
    beta = 1.0 / (1.0 + jnp.exp(-logit))
    gate = first * column(all_heads + tp * heads + head) + bias
    softplus = jnp.maximum(gate, 0.0) + jnp.log1p(jnp.exp(-jnp.abs(gate)))
    decay = jnp.exp(-jnp.exp(log_rate) * softplus)
    query_pre = first * total[:pairs]
    key_pre = first * total[pairs : 2 * pairs]
    value_pre = first * total[2 * pairs : 3 * pairs]
    query = query_pre * lax.rsqrt(jnp.sum(query_pre * query_pre, axis=1, keepdims=True) + epsilon)
    keyed = key_pre * lax.rsqrt(jnp.sum(key_pre * key_pre, axis=1, keepdims=True) + epsilon)
    both = jnp.concatenate([keyed, query], axis=0).astype(bf16)
    pair = lax.rem(lax.broadcasted_iota(jnp.int32, (2 * pairs, size), 0), pairs)
    reads = jnp.zeros((2 * pairs, size), f32)
    for r in range(pairs):
        reads = jnp.where(pair == r, dotted(both, states_low[r]), reads)
    fresh = beta * (value_pre - decay * reads[:pairs])
    overlap = jnp.sum(query * keyed, axis=1, keepdims=True)
    reading = decay * reads[pairs:] + overlap * fresh
    scale = lax.rsqrt(jnp.sum(reading * reading, axis=1, keepdims=True) / size + epsilon)
    norm_all[kv] = (reading * scale * gain_head[...]).astype(bf16)
    gather(over_kv, 1, kv, n_kv, norm_all)

    key_columns = keyed.T
    for r in range(pairs):
        b, h = r % seqs, r // seqs
        outer = key_columns[:, r : r + 1] * fresh[r : r + 1, :]
        new_state[b, h] = decay[r : r + 1, :] * states[b, h] + outer
    for name in ("out", "gain_two", "up", "down"):
        loads[name].wait()

    for off in range(1, n_kv):
        arrived(over_kv, 1, off, kv, n_kv, norm_all)
    normed = [norm_all[k].astype(f32) for k in range(n_kv)]
    normed = jnp.concatenate(
        [
            jnp.concatenate([x[h * seqs : (h + 1) * seqs] for x in normed], axis=0)
            for h in range(heads)
        ],
        axis=1,
    ).astype(bf16)
    part_all[tp] = dotted(normed, out_w[...]).astype(bf16)
    gather(over_tp, 1, tp, n_tp, part_all)
    for off in range(1, n_tp):
        arrived(over_tp, 1, off, tp, n_tp, part_all)
    attended = part_all[0].astype(f32)
    for t in range(1, n_tp):
        attended = attended + part_all[t].astype(f32)
    inputs = jnp.concatenate([token_all[t].astype(f32) for t in range(n_tp)], axis=1)
    middle = (inputs + attended).astype(bf16).astype(f32)
    for t in range(n_tp):
        middle_all[t] = middle[:, t * feats : (t + 1) * feats]
    square = jnp.sum(middle * middle, axis=1, keepdims=True)
    square_high = square.astype(bf16).astype(f32)
    lane = lax.broadcasted_iota(jnp.int32, (rows, 128), 1)
    square_pair = jnp.where(
        lane == 0, square_high, jnp.where(lane == 1, square - square_high, 0.0)
    ).astype(bf16)
    scaled = (middle * gain_two[...].astype(f32)).astype(bf16)

    def up_block(dest):
        at = pl.ds(pl.multiple_of(dest * share, share), share)
        return dotted(scaled, up_w[:, at])

    for off in range(1, n_kv):
        dest = lax.rem(kv + off, n_kv)
        up_send[off - 1, :, :share] = up_block(dest).astype(bf16)
        up_send[off - 1, :, share:] = square_pair
        copy = over_kv(2, off, up_send.at[off - 1], up_recv.at[off - 1])
        copy.start()
        sends.append(copy)
    up = up_block(kv)
    pair_sum = square_pair.astype(f32)
    for off in range(1, n_kv):
        over_kv(2, off, up_recv.at[off - 1], up_recv.at[off - 1]).wait_recv()
        up = up + up_recv[off - 1, :, :share].astype(f32)
        pair_sum = pair_sum + up_recv[off - 1, :, share:].astype(f32)
    second = lax.rsqrt(jnp.sum(pair_sum, axis=1, keepdims=True) / width + epsilon)
    hidden_all[kv] = jnp.square(jnp.maximum(second * up, 0.0)).astype(bf16)
    gather(over_kv, 3, kv, n_kv, hidden_all)

    def down_block(source):
        at = pl.ds(pl.multiple_of(source * share, share), share)
        return dotted(hidden_all[source], down_w[at, :])

    down = down_block(kv)
    for off in range(1, n_kv):
        down = down + down_block(arrived(over_kv, 3, off, kv, n_kv, hidden_all))
    for t in range(n_tp):
        down_send[t] = down[:, t * feats : (t + 1) * feats].astype(bf16)
    for off in range(1, n_tp):
        copy = over_tp(2, off, down_send.at[lax.rem(tp + off, n_tp)], down_recv.at[off - 1])
        copy.start()
        sends.append(copy)
    lowered = down_send[tp].astype(f32)
    for off in range(1, n_tp):
        over_tp(2, off, down_recv.at[off - 1], down_recv.at[off - 1]).wait_recv()
        lowered = lowered + down_recv[off - 1].astype(f32)
    mixed[...] = (middle_all[tp] + lowered).astype(bf16)
    for copy in sends:
        copy.wait_send()


def write_kernel(mixed_v, state_v, mixed, new_state, sem):
    copies = [
        pltpu.make_async_copy(mixed_v, mixed, sem.at[0]),
        pltpu.make_async_copy(state_v, new_state, sem.at[1]),
    ]
    for copy in copies:
        copy.start()
    for copy in copies:
        copy.wait()


def local(n_kv, n_tp, *arrays):
    tokens, state, w_beta, w_up = arrays[0], arrays[1], arrays[6], arrays[13]
    rows, feats = tokens.shape
    seqs, heads, size = state.shape[:3]
    pairs = seqs * heads
    share = w_up.shape[1] // n_kv
    aligned = (
        rows % 16 == 0
        and feats % 128 == 0
        and size == 128
        and pairs % 16 == 0
        and seqs <= 16
        and seqs * n_kv == rows
        and 2 * w_beta.shape[1] < 64
        and share % 128 == 0
        and n_kv > 1
        and n_tp > 1
    )
    if not aligned:
        return by_collectives(*arrays)
    block = n_tp * feats
    bf16, f32 = jnp.bfloat16, jnp.float32
    vmem = pltpu.VMEM

    def held(array):
        return vmem(array.shape, array.dtype)

    norm_gain, w_query, w_key, w_value = arrays[2:6]
    head_gain, w_out, mixer_gain, w_up, w_down = arrays[10:]
    dma = pltpu.SemaphoreType.DMA
    results = pl.pallas_call(
        functools.partial(layer_kernel, n_kv, n_tp),
        out_shape=(held(tokens), held(state)),
        in_specs=[pl.BlockSpec(memory_space=pltpu.HBM)] * len(arrays),
        out_specs=(pl.BlockSpec(memory_space=vmem),) * 2,
        scratch_shapes=[
            vmem((n_tp, rows, feats), bf16),
            held(norm_gain),
            held(mixer_gain),
            held(head_gain),
            held(w_query),
            held(w_key),
            held(w_value),
            vmem((w_beta.shape[1], block), bf16),
            vmem((w_beta.shape[1], block), bf16),
            held(w_out),
            held(w_up),
            held(w_down),
            held(state),
            vmem((pairs, size, size), bf16),
            pltpu.SMEM((heads,), f32),
            pltpu.SMEM((heads,), f32),
            vmem((n_kv, 3 * pairs + 16, size), bf16),
            vmem((n_kv - 1, 3 * pairs + 16, size), bf16),
            vmem((n_kv, pairs, size), bf16),
            vmem((n_tp, rows, block), bf16),
            vmem((n_tp, rows, feats), f32),
            vmem((n_kv - 1, rows, share + 128), bf16),
            vmem((n_kv - 1, rows, share + 128), bf16),
            vmem((n_kv, rows, share), bf16),
            vmem((n_tp, rows, feats), bf16),
            vmem((n_tp - 1, rows, feats), bf16),
            dma((15,)),
            dma((3, n_tp - 1)),
            dma((3, n_tp - 1)),
            dma((4, n_kv - 1)),
            dma((4, n_kv - 1)),
        ],
        compiler_params=pltpu.CompilerParams(
            collective_id=0, has_side_effects=True, vmem_limit_bytes=64 * 2**20 - 65536 - state.size * 4 - 2 * tokens.size
        ),
    )(*arrays[:6], arrays[6].T, arrays[7].T, *arrays[8:])
    return pl.pallas_call(
        write_kernel,
        out_shape=tuple(jax.ShapeDtypeStruct(r.shape, r.dtype) for r in (tokens, state)),
        in_specs=[pl.BlockSpec(memory_space=pl.ANY)] * 2,
        out_specs=(pl.BlockSpec(memory_space=pltpu.HBM),) * 2,
        scratch_shapes=[dma((2,))],
        compiler_params=pltpu.CompilerParams(vmem_limit_bytes=2**20),
    )(*results)


def solution(mesh):
    return jax.shard_map(
        functools.partial(local, mesh.shape["kv"], mesh.shape["tp"]),
        mesh=mesh,
        in_specs=(
            P("grp", ("kv", "tp")),
            P(("grp", "kv"), "tp", None, None),
            P("kv"),
            P("kv", "tp"),
            P("kv", "tp"),
            P("kv", "tp"),
            P(),
            P(),
            P("tp"),
            P("tp"),
            P(),
            P("tp", "kv"),
            P("kv"),
            P("kv", "tp"),
            P("tp", "kv"),
        ),
        out_specs=(P("grp", ("kv", "tp")), P(("grp", "kv"), "tp", None, None)),
        check_vma=False,
    )
```

```python
import functools

import jax
import jax.numpy as jnp
from jax import lax
from jax.experimental import pallas as pl
from jax.experimental.pallas import tpu as pltpu
from jax.sharding import PartitionSpec as P

MESH = pl.DeviceIdType.MESH

epsilon = 1e-06


def dotted(left, right):
    return jnp.dot(left, right, preferred_element_type=jnp.float32)


def delta_update(
    query_pre, key_pre, value_pre, beta_pre, decay_pre, state, a_log, dt_bias, head_gain
):
    query = query_pre * lax.rsqrt(jnp.sum(query_pre * query_pre, axis=-1, keepdims=True) + epsilon)
    keyed = key_pre * lax.rsqrt(jnp.sum(key_pre * key_pre, axis=-1, keepdims=True) + epsilon)
    beta = jax.nn.sigmoid(beta_pre)
    decay = jnp.exp(-jnp.exp(a_log) * jax.nn.softplus(decay_pre + dt_bias))
    key_read = jnp.einsum("bhk,bhkv->bhv", keyed, state)
    query_read = jnp.einsum("bhk,bhkv->bhv", query, state)
    fresh = beta[..., None] * (value_pre - decay[..., None] * key_read)
    new_state = decay[..., None, None] * state + keyed[..., :, None] * fresh[..., None, :]
    intersection = jnp.sum(query * keyed, axis=-1)
    reading = decay[..., None] * query_read + intersection[..., None] * fresh
    normed = (
        reading
        * lax.rsqrt(jnp.mean(reading * reading, axis=-1, keepdims=True) + epsilon)
        * head_gain
    )
    return (normed.astype(jnp.bfloat16), new_state)


def by_collectives(
    tokens,
    state,
    norm_gain,
    w_query,
    w_key,
    w_value,
    w_beta,
    w_decay,
    a_log,
    dt_bias,
    head_gain,
    w_out,
    mixer_gain,
    w_up,
    w_down,
):
    seq_here = state.shape[0]
    heads_here = state.shape[1]
    head_size = state.shape[2]
    kv_index = lax.axis_index("kv")
    tp_index = lax.axis_index("tp")
    gathered = lax.all_gather(tokens, "tp", axis=1, tiled=True)
    block = gathered.shape[1]
    width = block * lax.axis_size("kv")
    inputs = gathered.astype(jnp.float32)
    scaled = (inputs * norm_gain.astype(jnp.float32)).astype(jnp.bfloat16)
    partial_sq = jnp.sum(inputs * inputs, axis=1)
    beta_rows = lax.dynamic_slice(
        w_beta, (kv_index * block, tp_index * heads_here), (block, heads_here)
    )
    decay_rows = lax.dynamic_slice(
        w_decay, (kv_index * block, tp_index * heads_here), (block, heads_here)
    )
    query_part = dotted(scaled, w_query)
    key_part = dotted(scaled, w_key)
    value_part = dotted(scaled, w_value)
    beta_part = dotted(scaled, beta_rows)
    decay_part = dotted(scaled, decay_rows)
    square_all = lax.psum(partial_sq, "kv")
    square_sum = lax.dynamic_slice_in_dim(square_all, kv_index * seq_here, seq_here, 0)
    query_sum, key_sum, value_sum, beta_sum, decay_sum = (
        lax.psum_scatter(query_part, "kv", scatter_dimension=0, tiled=True),
        lax.psum_scatter(key_part, "kv", scatter_dimension=0, tiled=True),
        lax.psum_scatter(value_part, "kv", scatter_dimension=0, tiled=True),
        lax.psum_scatter(beta_part, "kv", scatter_dimension=0, tiled=True),
        lax.psum_scatter(decay_part, "kv", scatter_dimension=0, tiled=True),
    )
    first = lax.rsqrt(square_sum / width + epsilon)[:, None]
    query_pre = (first * query_sum).reshape(seq_here, heads_here, head_size)
    key_pre = (first * key_sum).reshape(seq_here, heads_here, head_size)
    value_pre = (first * value_sum).reshape(seq_here, heads_here, head_size)
    normed, new_state = delta_update(
        query_pre,
        key_pre,
        value_pre,
        first * beta_sum,
        first * decay_sum,
        state,
        a_log,
        dt_bias,
        head_gain,
    )
    normed = normed.reshape(seq_here, heads_here * head_size)
    head_part = dotted(lax.all_gather(normed, "kv", axis=0, tiled=True), w_out)
    attended = lax.psum_scatter(
        head_part.astype(jnp.bfloat16), "tp", scatter_dimension=1, tiled=True
    ).astype(jnp.float32)
    middle = (tokens.astype(jnp.float32) + attended).astype(jnp.bfloat16)
    middle_rows = lax.all_gather(middle, "tp", axis=1, tiled=True).astype(jnp.float32)
    square_two = lax.psum(jnp.sum(middle_rows * middle_rows, axis=1), "kv")
    second = lax.rsqrt(square_two / width + epsilon)[:, None]
    scaled_two = (middle_rows * mixer_gain.astype(jnp.float32)).astype(jnp.bfloat16)
    up_part = dotted(scaled_two, w_up)
    up_share = lax.psum_scatter(up_part, "kv", scatter_dimension=1, tiled=True)
    hidden_share = jnp.square(jax.nn.relu(second * up_share)).astype(jnp.bfloat16)
    down_part = dotted(lax.all_gather(hidden_share, "kv", axis=1, tiled=True), w_down)
    lowered = lax.psum_scatter(
        down_part.astype(jnp.bfloat16), "tp", scatter_dimension=1, tiled=True
    ).astype(jnp.float32)
    mixed = (middle.astype(jnp.float32) + lowered).astype(jnp.bfloat16)
    return (mixed, new_state)


def across(left, right):
    return lax.dot_general(
        left, right, (((1,), (1,)), ((), ())), preferred_element_type=jnp.float32
    )


def layer_kernel(
    n_kv,
    n_tp,
    tokens,
    state,
    norm_gain,
    w_query,
    w_key,
    w_value,
    w_beta,
    w_decay,
    a_log,
    dt_bias,
    head_gain,
    w_out,
    mixer_gain,
    w_up,
    w_down,
    mixed,
    new_state,
    token_all,
    gain_one,
    gain_two,
    gain_head,
    query_w,
    key_w,
    value_w,
    beta_w,
    decay_w,
    out_w,
    up_w,
    down_w,
    states,
    states_low,
    log_s,
    bias_s,
    qkv_send,
    qkv_recv,
    norm_all,
    part_all,
    middle_all,
    up_send,
    up_recv,
    hidden_all,
    down_send,
    down_recv,
    load_sem,
    tp_send_sem,
    tp_recv_sem,
    kv_send_sem,
    kv_recv_sem,
    news_sem,
):
    f32, bf16 = jnp.float32, jnp.bfloat16
    kv = lax.axis_index("kv")
    tp = lax.axis_index("tp")
    rows, feats = tokens.shape
    block = n_tp * feats
    seqs, heads, size = state.shape[:3]
    pairs = seqs * heads
    all_heads = w_beta.shape[0]
    share = w_up.shape[1] // n_kv
    width = block * n_kv

    barrier = pltpu.get_barrier_semaphore()
    for off in range(1, n_tp):
        pl.semaphore_signal(
            barrier, inc=1, device_id={"tp": lax.rem(tp + off, n_tp)}, device_id_type=MESH
        )
    last = n_kv - 1
    for step in (-1, 1):

        @pl.when((kv + step >= 0) & (kv + step <= last))
        def _(step=step):
            pl.semaphore_signal(barrier, inc=1, device_id={"kv": kv + step}, device_id_type=MESH)

    turn = jnp.where(2 * kv >= n_kv, 1, -1)
    kv_offs = [lax.rem(n_kv + turn * j, n_kv) for j in range(1, n_kv)]

    def tell(far):
        for side, step in enumerate((-1, 1)):

            @pl.when((kv + step >= 0) & (kv + step <= last))
            def _(side=side, step=step):
                @pl.when((kv - far * step >= 0) & (kv - far * step <= last))
                def _():
                    pl.semaphore_signal(
                        news_sem.at[far - 1, side],
                        inc=1,
                        device_id={"kv": kv + step},
                        device_id_type=MESH,
                    )

    def hear(far):
        for side, step in enumerate((-1, 1)):

            @pl.when((kv - (far + 1) * step >= 0) & (kv - (far + 1) * step <= last))
            def _(side=side):
                pl.semaphore_wait(news_sem.at[far - 1, side], 1)

    my_rows = pl.ds(pl.multiple_of(kv * block, block), block)
    loads = {}
    for number, (name, source, target) in enumerate(
        (
            ("tokens", tokens, token_all.at[tp]),
            ("gain_one", norm_gain, gain_one),
            ("query", w_query, query_w),
            ("key", w_key, key_w),
            ("value", w_value, value_w),
            ("beta", w_beta.at[:, my_rows], beta_w),
            ("decay", w_decay.at[:, my_rows], decay_w),
            ("log", a_log, log_s),
            ("bias", dt_bias, bias_s),
            ("gain_head", head_gain, gain_head),
            ("state", state, states),
            ("out", w_out, out_w),
            ("gain_two", mixer_gain, gain_two),
            ("up", w_up, up_w),
            ("down", w_down, down_w),
        )
    ):
        loads[name] = pltpu.make_async_copy(source, target, load_sem.at[number])
        loads[name].start()

    sends = []

    def over_tp(stage, off, source, target):
        copy = pltpu.make_async_remote_copy(
            src_ref=source,
            dst_ref=target,
            send_sem=tp_send_sem.at[stage, off - 1],
            recv_sem=tp_recv_sem.at[stage, off - 1],
            device_id={"tp": lax.rem(tp + off, n_tp)},
            device_id_type=MESH,
        )
        return copy

    def over_kv(stage, off, source, target):
        copy = pltpu.make_async_remote_copy(
            src_ref=source,
            dst_ref=target,
            send_sem=kv_send_sem.at[stage, off - 1],
            recv_sem=kv_recv_sem.at[stage, off - 1],
            device_id={"kv": lax.rem(kv + off, n_kv)},
            device_id_type=MESH,
        )
        return copy

    def gather(over, stage, here, offs, slots):
        for off in offs:
            copy = over(stage, off, slots.at[here], slots.at[here])
            copy.start()
            sends.append(copy)

    def arrived(over, stage, off, here, count, slots):
        origin = lax.rem(here + count - off, count)
        over(stage, off, slots.at[origin], slots.at[origin]).wait_recv()
        return origin

    loads["tokens"].wait()
    neighbours = jnp.where(kv > 0, 1, 0) + jnp.where(kv < last, 1, 0)
    pl.semaphore_wait(barrier, n_tp - 1 + neighbours)

    gather(over_tp, 0, tp, range(1, n_tp), token_all)
    for far in range(1, n_kv - 1):
        tell(far)
        if far < n_kv - 2:
            hear(far)
    for name in ("gain_one", "query", "key", "value", "beta", "decay", "log", "bias", "gain_head"):
        loads[name].wait()
    for off in range(1, n_tp):
        arrived(over_tp, 0, off, tp, n_tp, token_all)
    inputs = jnp.concatenate([token_all[t].astype(f32) for t in range(n_tp)], axis=1)
    scaled = (inputs * gain_one[...].astype(f32)).astype(bf16)
    square = jnp.sum(inputs * inputs, axis=1, keepdims=True)
    side = jnp.concatenate(
        [
            across(scaled, beta_w[...]),
            across(scaled, decay_w[...]),
            square,
            jnp.zeros((rows, 64 - 2 * all_heads - 1), f32),
        ],
        axis=1,
    )
    side_high = side.astype(bf16).astype(f32)
    side = jnp.concatenate([side_high, side - side_high], axis=1)
    parts = [dotted(scaled, w[...]) for w in (query_w, key_w, value_w)]
    pad = jnp.zeros((16 - seqs, 128), f32)
    for dest in range(n_kv):
        at = slice(dest * seqs, (dest + 1) * seqs)
        pieces = [p[at, h * size : (h + 1) * size] for p in parts for h in range(heads)]
        qkv_send[dest] = jnp.concatenate(pieces + [side[at], pad], axis=0).astype(bf16)
    if n_kv > 2:
        hear(n_kv - 2)
    for off in kv_offs:
        copy = over_kv(0, off, qkv_send.at[lax.rem(kv + off, n_kv)], qkv_recv.at[off - 1])
        copy.start()
        sends.append(copy)

    loads["state"].wait()
    for b in range(seqs):
        for h in range(heads):
            states_low[h * seqs + b] = states[b, h].astype(bf16)
    total = qkv_send[kv].astype(f32)
    for off in kv_offs:
        over_kv(0, off, qkv_recv.at[off - 1], qkv_recv.at[off - 1]).wait_recv()
        total = total + qkv_recv[off - 1].astype(f32)

    lane = lax.rem(lax.broadcasted_iota(jnp.int32, (pairs, 128), 1), 64)
    head = lax.broadcasted_iota(jnp.int32, (pairs, 128), 0) // seqs
    side = jnp.concatenate([total[3 * pairs : 3 * pairs + seqs]] * heads, axis=0)

    def column(index):
        return jnp.sum(jnp.where(lane == index, side, 0.0), axis=1, keepdims=True)

    head_one = lax.broadcasted_iota(jnp.int32, (pairs, 1), 0) // seqs
    log_rate = jnp.zeros((pairs, 1), f32)
    bias = jnp.zeros((pairs, 1), f32)
    for h in range(heads):
        log_rate = jnp.where(head_one == h, log_s[h], log_rate)
        bias = jnp.where(head_one == h, bias_s[h], bias)
    first = lax.rsqrt(column(2 * all_heads) / width + epsilon)
    logit = first * column(tp * heads + head)
    beta = 1.0 / (1.0 + jnp.exp(-logit))
    gate = first * column(all_heads + tp * heads + head) + bias
    softplus = jnp.maximum(gate, 0.0) + jnp.log1p(jnp.exp(-jnp.abs(gate)))
    decay = jnp.exp(-jnp.exp(log_rate) * softplus)
    query_pre = first * total[:pairs]
    key_pre = first * total[pairs : 2 * pairs]
    value_pre = first * total[2 * pairs : 3 * pairs]
    query = query_pre * lax.rsqrt(jnp.sum(query_pre * query_pre, axis=1, keepdims=True) + epsilon)
    keyed = key_pre * lax.rsqrt(jnp.sum(key_pre * key_pre, axis=1, keepdims=True) + epsilon)
    both = jnp.concatenate([keyed, query], axis=0).astype(bf16)
    pair = lax.rem(lax.broadcasted_iota(jnp.int32, (2 * pairs, size), 0), pairs)
    reads = jnp.zeros((2 * pairs, size), f32)
    for r in range(pairs):
        reads = jnp.where(pair == r, dotted(both, states_low[r]), reads)
    fresh = beta * (value_pre - decay * reads[:pairs])
    overlap = jnp.sum(query * keyed, axis=1, keepdims=True)
    reading = decay * reads[pairs:] + overlap * fresh
    scale = lax.rsqrt(jnp.sum(reading * reading, axis=1, keepdims=True) / size + epsilon)
    norm_all[kv] = (reading * scale * gain_head[...]).astype(bf16)
    gather(over_kv, 1, kv, kv_offs, norm_all)

    key_columns = keyed.T
    for r in range(pairs):
        b, h = r % seqs, r // seqs
        outer = key_columns[:, r : r + 1] * fresh[r : r + 1, :]
        new_state[b, h] = decay[r : r + 1, :] * states[b, h] + outer
    for name in ("out", "gain_two", "up", "down"):
        loads[name].wait()

    for off in range(1, n_kv):
        arrived(over_kv, 1, off, kv, n_kv, norm_all)
    normed = [norm_all[k].astype(f32) for k in range(n_kv)]
    normed = jnp.concatenate(
        [
            jnp.concatenate([x[h * seqs : (h + 1) * seqs] for x in normed], axis=0)
            for h in range(heads)
        ],
        axis=1,
    ).astype(bf16)
    part_all[tp] = dotted(normed, out_w[...]).astype(bf16)
    gather(over_tp, 1, tp, range(1, n_tp), part_all)
    for off in range(1, n_tp):
        arrived(over_tp, 1, off, tp, n_tp, part_all)
    attended = part_all[0].astype(f32)
    for t in range(1, n_tp):
        attended = attended + part_all[t].astype(f32)
    inputs = jnp.concatenate([token_all[t].astype(f32) for t in range(n_tp)], axis=1)
    middle = (inputs + attended).astype(bf16).astype(f32)
    for t in range(n_tp):
        middle_all[t] = middle[:, t * feats : (t + 1) * feats]
    square = jnp.sum(middle * middle, axis=1, keepdims=True)
    square_high = square.astype(bf16).astype(f32)
    lane = lax.broadcasted_iota(jnp.int32, (rows, 128), 1)
    square_pair = jnp.where(
        lane == 0, square_high, jnp.where(lane == 1, square - square_high, 0.0)
    ).astype(bf16)
    scaled = (middle * gain_two[...].astype(f32)).astype(bf16)

    def up_block(dest):
        at = pl.ds(pl.multiple_of(dest * share, share), share)
        return dotted(scaled, up_w[:, at])

    for off in kv_offs:
        dest = lax.rem(kv + off, n_kv)
        up_send[off - 1, :, :share] = up_block(dest).astype(bf16)
        up_send[off - 1, :, share:] = square_pair
        copy = over_kv(2, off, up_send.at[off - 1], up_recv.at[off - 1])
        copy.start()
        sends.append(copy)
    up = up_block(kv)
    pair_sum = square_pair.astype(f32)
    for off in kv_offs:
        over_kv(2, off, up_recv.at[off - 1], up_recv.at[off - 1]).wait_recv()
        up = up + up_recv[off - 1, :, :share].astype(f32)
        pair_sum = pair_sum + up_recv[off - 1, :, share:].astype(f32)
    second = lax.rsqrt(jnp.sum(pair_sum, axis=1, keepdims=True) / width + epsilon)
    hidden_all[kv] = jnp.square(jnp.maximum(second * up, 0.0)).astype(bf16)
    gather(over_kv, 3, kv, kv_offs, hidden_all)

    def down_block(source):
        at = pl.ds(pl.multiple_of(source * share, share), share)
        return dotted(hidden_all[source], down_w[at, :])

    down = down_block(kv)
    for off in kv_offs:
        down = down + down_block(arrived(over_kv, 3, off, kv, n_kv, hidden_all))
    for t in range(n_tp):
        down_send[t] = down[:, t * feats : (t + 1) * feats].astype(bf16)
    for off in range(1, n_tp):
        copy = over_tp(2, off, down_send.at[lax.rem(tp + off, n_tp)], down_recv.at[off - 1])
        copy.start()
        sends.append(copy)
    lowered = down_send[tp].astype(f32)
    for off in range(1, n_tp):
        over_tp(2, off, down_recv.at[off - 1], down_recv.at[off - 1]).wait_recv()
        lowered = lowered + down_recv[off - 1].astype(f32)
    mixed[...] = (middle_all[tp] + lowered).astype(bf16)
    for copy in sends:
        copy.wait_send()


def write_kernel(mixed_v, state_v, mixed, new_state, sem):
    copies = [
        pltpu.make_async_copy(mixed_v, mixed, sem.at[0]),
        pltpu.make_async_copy(state_v, new_state, sem.at[1]),
    ]
    for copy in copies:
        copy.start()
    for copy in copies:
        copy.wait()


def local(n_kv, n_tp, *arrays):
    tokens, state, w_beta, w_up = arrays[0], arrays[1], arrays[6], arrays[13]
    rows, feats = tokens.shape
    seqs, heads, size = state.shape[:3]
    pairs = seqs * heads
    share = w_up.shape[1] // n_kv
    aligned = (
        rows % 16 == 0
        and feats % 128 == 0
        and size == 128
        and pairs % 16 == 0
        and seqs <= 16
        and seqs * n_kv == rows
        and 2 * w_beta.shape[1] < 64
        and share % 128 == 0
        and n_kv > 1
        and n_tp > 1
    )
    if not aligned:
        return by_collectives(*arrays)
    block = n_tp * feats
    bf16, f32 = jnp.bfloat16, jnp.float32
    vmem = pltpu.VMEM

    def held(array):
        return vmem(array.shape, array.dtype)

    norm_gain, w_query, w_key, w_value = arrays[2:6]
    head_gain, w_out, mixer_gain, w_up, w_down = arrays[10:]
    dma = pltpu.SemaphoreType.DMA
    results = pl.pallas_call(
        functools.partial(layer_kernel, n_kv, n_tp),
        out_shape=(held(tokens), held(state)),
        in_specs=[pl.BlockSpec(memory_space=pltpu.HBM)] * len(arrays),
        out_specs=(pl.BlockSpec(memory_space=vmem),) * 2,
        scratch_shapes=[
            vmem((n_tp, rows, feats), bf16),
            held(norm_gain),
            held(mixer_gain),
            held(head_gain),
            held(w_query),
            held(w_key),
            held(w_value),
            vmem((w_beta.shape[1], block), bf16),
            vmem((w_beta.shape[1], block), bf16),
            held(w_out),
            held(w_up),
            held(w_down),
            held(state),
            vmem((pairs, size, size), bf16),
            pltpu.SMEM((heads,), f32),
            pltpu.SMEM((heads,), f32),
            vmem((n_kv, 3 * pairs + 16, size), bf16),
            vmem((n_kv - 1, 3 * pairs + 16, size), bf16),
            vmem((n_kv, pairs, size), bf16),
            vmem((n_tp, rows, block), bf16),
            vmem((n_tp, rows, feats), f32),
            vmem((n_kv - 1, rows, share + 128), bf16),
            vmem((n_kv - 1, rows, share + 128), bf16),
            vmem((n_kv, rows, share), bf16),
            vmem((n_tp, rows, feats), bf16),
            vmem((n_tp - 1, rows, feats), bf16),
            dma((15,)),
            dma((3, n_tp - 1)),
            dma((3, n_tp - 1)),
            dma((4, n_kv - 1)),
            dma((4, n_kv - 1)),
            pltpu.SemaphoreType.REGULAR((max(n_kv - 2, 1), 2)),
        ],
        compiler_params=pltpu.CompilerParams(
            collective_id=0, has_side_effects=True, vmem_limit_bytes=64 * 2**20 - 65536 - state.size * 4 - 2 * tokens.size
        ),
    )(*arrays[:6], arrays[6].T, arrays[7].T, *arrays[8:])
    return pl.pallas_call(
        write_kernel,
        out_shape=tuple(jax.ShapeDtypeStruct(r.shape, r.dtype) for r in (tokens, state)),
        in_specs=[pl.BlockSpec(memory_space=pl.ANY)] * 2,
        out_specs=(pl.BlockSpec(memory_space=pltpu.HBM),) * 2,
        scratch_shapes=[dma((2,))],
        compiler_params=pltpu.CompilerParams(vmem_limit_bytes=2**20),
    )(*results)


def solution(mesh):
    return jax.shard_map(
        functools.partial(local, mesh.shape["kv"], mesh.shape["tp"]),
        mesh=mesh,
        in_specs=(
            P("grp", ("kv", "tp")),
            P(("grp", "kv"), "tp", None, None),
            P("kv"),
            P("kv", "tp"),
            P("kv", "tp"),
            P("kv", "tp"),
            P(),
            P(),
            P("tp"),
            P("tp"),
            P(),
            P("tp", "kv"),
            P("kv"),
            P("kv", "tp"),
            P("tp", "kv"),
        ),
        out_specs=(P("grp", ("kv", "tp")), P(("grp", "kv"), "tp", None, None)),
        check_vma=False,
    )
```
